32 devices in a mesh: pp: 4 (over z), fs: 2 (over y), tp: 4 (over x, core).
Axes of the slice: x: 2, y: 2, z: 4, core: 2. Of those that a mesh axis runs over, the one named last changes fastest.
Arguments:
- tokens_in: bfloat16 [4, 8, 8, 2048], P('pp', ('fs', 'tp')), may hold values from -6 to 6
- weight_in: bfloat16 [4, 2048, 512], P('pp'), may hold values from -0.125 to 0.125
- conv_taps: float32 [4, 4, 512], P('pp'), may hold values from -3 to 3
- conv_bias: float32 [4, 512], P('pp'), may hold values from -2 to 2
- gate_rate: bfloat16 [4, 8, 64, 64], P('pp'), may hold values from -0.75 to 0.75
- bias_rate: float32 [4, 512], P('pp'), may hold values from -3 to 3
- gate_input: bfloat16 [4, 8, 64, 64], P('pp'), may hold values from -0.75 to 0.75
- bias_input: float32 [4, 512], P('pp'), may hold values from -3 to 3
- decay_param: float32 [4, 512], P('pp'), may hold values from 3.5 to 7.5
- weight_out: bfloat16 [4, 512, 2048], P('pp'), may hold values from -0.5 to 0.5
- norm_gain: float32 [4, 2048], P('pp'), may hold values from 0.1 to 1.9
- norm_shift: float32 [4, 2048], P('pp'), may hold values from -2 to 2
Outputs:
- tokens_out: bfloat16 [4, 8, 8, 2048], P('pp', ('fs', 'tp'))
The draws below stay inside these ranges and needn't reach their ends.
All inputs are finite; a program needn't handle non-finite values.
Results may differ from the reference program's by a relative error of at most 0.022.
Values may be sent and summed in bfloat16 or wider, within the bound.
A program may use at most 128 MiB of HBM per device.

```python
import jax
import jax.numpy as jnp
from jax import lax

D = 2048
LRU_W = 512
LRU_BLOCKS = 8
BLOCK_W = 64
CONV = 4
LEN = 8
SECTIONS = 4
SEQS = 8


def shard_levels(stream_key, shape, pieces, least, largest):
    def one(axis_at, shards_of):
        draws = jax.random.uniform(jax.random.fold_in(jax.random.fold_in(stream_key, 6), axis_at), (shards_of,), jnp.float32, least / len(pieces), largest / len(pieces))
        return jnp.repeat(jnp.exp(draws), shape[axis_at] // shards_of).reshape((-1,) + (1,) * (len(shape) - axis_at - 1))

    gain = one(*pieces[0])
    for cut in pieces[1:]:
        gain = gain * one(*cut)
    return gain


def centred(stream_key, shape, spread, bound, pieces=(), kind=jnp.bfloat16):
    factor_of = shard_levels(stream_key, shape, pieces, -0.22, 0.18) if pieces else 1.0
    entries = jax.random.normal(stream_key, shape, jnp.float32) * spread * factor_of
    return jnp.minimum(jnp.maximum(entries, -bound), bound).astype(kind)


def setup_inputs(seed: int = 0) -> dict:
    streams_of = jax.random.split(jax.random.key(seed), 13)
    tokens_in = centred(streams_of[0], (SECTIONS, SEQS, LEN, D), 1.0, 6.0, ((0, 4), (1, 8)))
    weight_in = centred(streams_of[1], (SECTIONS, D, LRU_W), D ** -0.5, 0.125, ((0, 4),))
    conv_taps = centred(streams_of[2], (SECTIONS, CONV, LRU_W), 0.5, 3.0, ((0, 4),), jnp.float32)
    conv_bias = centred(streams_of[3], (SECTIONS, LRU_W), 0.3, 2.0, ((0, 4),), jnp.float32)
    gate_rate = centred(streams_of[4], (SECTIONS, LRU_BLOCKS, BLOCK_W, BLOCK_W), BLOCK_W ** -0.5, 0.75, ((0, 4),))
    bias_rate = centred(streams_of[5], (SECTIONS, LRU_W), 0.5, 3.0, ((0, 4),), jnp.float32)
    gate_input = centred(streams_of[6], (SECTIONS, LRU_BLOCKS, BLOCK_W, BLOCK_W), BLOCK_W ** -0.5, 0.75, ((0, 4),))
    bias_input = centred(streams_of[7], (SECTIONS, LRU_W), 0.5, 3.0, ((0, 4),), jnp.float32)
    decay_param = jnp.clip(3.5 + 4.0 * jax.random.uniform(streams_of[8], (SECTIONS, LRU_W), jnp.float32) ** shard_levels(streams_of[8], (SECTIONS, LRU_W), ((0, 4),), -0.2, 0.2), 3.5, 7.5)
    weight_out = centred(streams_of[9], (SECTIONS, LRU_W, D), (LRU_W // 4) ** -0.5, 0.5, ((0, 4),))
    norm_gain = jnp.clip(1.0 + 0.18 * jax.random.normal(streams_of[10], (SECTIONS, D), jnp.float32), 0.1, 1.9)
    norm_shift = centred(streams_of[11], (SECTIONS, D), 0.3, 2.0, ((0, 4),), jnp.float32)
    return dict(tokens_in=tokens_in, weight_in=weight_in, conv_taps=conv_taps, conv_bias=conv_bias, gate_rate=gate_rate, bias_rate=bias_rate, gate_input=gate_input, bias_input=bias_input, decay_param=decay_param, weight_out=weight_out, norm_gain=norm_gain, norm_shift=norm_shift)


decay_scale = 8.0
norm_eps = 1e-05

def combine_steps(earlier, later):
    return (earlier[0] * later[0], later[0] * earlier[1] + later[1])

def recurrence(projected, conv_taps, conv_bias, gate_rate, bias_rate, gate_input, bias_input, decay_param):
    seq_count, length, channels = projected.shape
    tap_count = conv_taps.shape[0]
    padded = jnp.pad(projected.astype(jnp.float32), ((0, 0), (tap_count - 1, 0), (0, 0)))
    convolved = conv_bias + padded[:, 0:length] * conv_taps[0]
    for tap_index in range(1, tap_count):
        convolved = convolved + padded[:, tap_index:tap_index + length] * conv_taps[tap_index]
    convolved = convolved.astype(jnp.bfloat16)
    blocks = gate_rate.shape[0]
    block_width = gate_rate.shape[1]
    grouped = convolved.astype(jnp.float32).reshape(seq_count, length, blocks, block_width)
    rate_pre = jnp.einsum('bsnc,ncd->bsnd', grouped, gate_rate.astype(jnp.float32))
    input_pre = jnp.einsum('bsnc,ncd->bsnd', grouped, gate_input.astype(jnp.float32))
    rate_gate = jax.nn.sigmoid(rate_pre.reshape(seq_count, length, channels) + bias_rate)
    input_gate = jax.nn.sigmoid(input_pre.reshape(seq_count, length, channels) + bias_input)
    log_decay = -decay_scale * rate_gate * jax.nn.softplus(-decay_param)
    scale_in = jnp.sqrt(-jnp.expm1(2.0 * log_decay))
    driven = scale_in * input_gate * convolved.astype(jnp.float32)
    decay_now = jnp.exp(log_decay)
    unused, hidden = lax.associative_scan(combine_steps, (decay_now, driven), axis=1)
    return hidden.astype(jnp.bfloat16)

def finish(stream_rows, mixed_rows, weight_out, norm_gain, norm_shift):
    summed = stream_rows.astype(jnp.float32) + jnp.dot(mixed_rows, weight_out, preferred_element_type=jnp.float32)
    mean_value = lax.optimization_barrier(jnp.mean(summed, axis=-1, keepdims=True))
    centered = summed - mean_value
    variance = lax.optimization_barrier(jnp.mean(centered * centered, axis=-1, keepdims=True))
    return (centered * lax.rsqrt(variance + norm_eps) * norm_gain + norm_shift).astype(jnp.bfloat16)

def reference(tokens_in, weight_in, conv_taps, conv_bias, gate_rate, bias_rate, gate_input, bias_input, decay_param, weight_out, norm_gain, norm_shift):
    length = tokens_in.shape[2]
    model_width = tokens_in.shape[3]
    stream = tokens_in.reshape(-1, length, model_width)
    seq_count = stream.shape[0]

    def apply_section(current, section_weights):
        w_project, taps_now, cbias_now, grate_now, brate_now, ginput_now, binput_now, dparam_now, w_back, gain_now, shift_now = section_weights
        lru_width = w_project.shape[1]
        flat_rows = current.reshape(seq_count * length, model_width)
        projected = jnp.dot(flat_rows, w_project, preferred_element_type=jnp.float32).astype(jnp.bfloat16)
        projected = projected.reshape(seq_count, length, lru_width)
        mixed_out = recurrence(projected, taps_now, cbias_now, grate_now, brate_now, ginput_now, binput_now, dparam_now)
        result = finish(flat_rows, mixed_out.reshape(seq_count * length, lru_width), w_back, gain_now, shift_now)
        return (result.reshape(seq_count, length, model_width), None)
    stream, unused = lax.scan(apply_section, stream, (weight_in, conv_taps, conv_bias, gate_rate, bias_rate, gate_input, bias_input, decay_param, weight_out, norm_gain, norm_shift))
    return stream.reshape(tokens_in.shape)
```

```python
import functools

import jax
import jax.numpy as jnp
from jax import lax
from jax.experimental import pallas as pl
from jax.experimental.pallas import tpu as pltpu
from jax.sharding import PartitionSpec as P

decay_scale = 8.0
norm_eps = 1e-05
mxu_width = 256
MESH = pl.DeviceIdType.MESH


def stack_kernel(
    sections,
    tokens_hbm,
    w_in_hbm,
    taps_hbm,
    cbias_hbm,
    grate_hbm,
    brate_hbm,
    ginput_hbm,
    binput_hbm,
    dparam_hbm,
    w_out_hbm,
    gain_hbm,
    shift_hbm,
    out_ref,
    w_in,
    w_out,
    taps,
    cbias,
    grate,
    brate,
    ginput,
    binput,
    dparam,
    gain,
    shift,
    rate_map,
    input_map,
    inbox,
    outbox,
    load_sem,
    entry_sem,
    send_sem,
    recv_sem,
    final_sem,
):
    section = lax.axis_index("pp")
    last = sections - 1
    length = inbox.shape[1]
    lru_width = w_in.shape[1]

    def other(offset):
        return lax.rem(section + offset, sections)

    barrier = pltpu.get_barrier_semaphore()
    for offset in range(1, sections):
        pl.semaphore_signal(
            barrier, inc=1, device_id={"pp": other(offset)}, device_id_type=MESH
        )

    def load(src, dst, index):
        return pltpu.make_async_copy(src, dst, load_sem.at[index])

    own = load(tokens_hbm.at[0, 0], inbox.at[0], 0)
    load_in = load(w_in_hbm.at[0], w_in, 1)
    load_out = load(w_out_hbm.at[0], w_out, 2)
    small = [
        load(grate_hbm.at[0], grate, 3),
        load(ginput_hbm.at[0], ginput, 4),
        load(taps_hbm.at[0], taps, 5),
        load(cbias_hbm, cbias, 6),
        load(brate_hbm, brate, 7),
        load(binput_hbm, binput, 8),
        load(dparam_hbm, dparam, 9),
        load(gain_hbm, gain, 10),
        load(shift_hbm, shift, 11),
    ]

    @pl.when(section == 0)
    def _():
        own.start()

    for copy in small:
        copy.start()
    load_in.start()
    load_out.start()

    for copy in small:
        copy.wait()
    blocks, block_width, _ = grate.shape
    group = max(1, min(blocks, mxu_width // block_width))
    wide = group * block_width
    rate_map[...] = jnp.zeros_like(rate_map)
    input_map[...] = jnp.zeros_like(input_map)
    for block in range(blocks):
        at = (block % group) * block_width
        rate_map[block // group, at : at + block_width, at : at + block_width] = grate[block]
        input_map[block // group, at : at + block_width, at : at + block_width] = ginput[block]
    minus_decay = -dparam[...]
    softplus = jnp.maximum(minus_decay, 0.0) + jnp.log1p(jnp.exp(-jnp.abs(minus_decay)))
    dparam[...] = -decay_scale * softplus

    entry = pltpu.make_async_remote_copy(
        src_ref=tokens_hbm.at[0, 0],
        dst_ref=inbox.at[section],
        send_sem=entry_sem,
        recv_sem=recv_sem.at[section],
        device_id={"pp": 0},
        device_id_type=MESH,
    )

    @pl.when(section > 0)
    def _():
        pl.semaphore_wait(barrier, sections - 1)
        entry.start()

    load_in.wait()
    load_out.wait()

    position = lax.broadcasted_iota(jnp.int32, (length, lru_width), 0)

    def delayed(x, by, fill):
        return jnp.where(position >= by, pltpu.roll(x, by, 0), fill)

    def onward(slot):
        return pltpu.make_async_remote_copy(
            src_ref=outbox.at[slot],
            dst_ref=inbox.at[slot],
            send_sem=send_sem.at[slot],
            recv_sem=recv_sem.at[slot],
            device_id={"pp": jnp.minimum(section + 1, last)},
            device_id_type=MESH,
        )

    def home(slot):
        return pltpu.make_async_remote_copy(
            src_ref=outbox.at[slot],
            dst_ref=out_ref.at[0, 0],
            send_sem=send_sem.at[slot],
            recv_sem=final_sem,
            device_id={"pp": slot},
            device_id_type=MESH,
        )

    def one_slot(slot, carry):
        from_here = (section == 0) & (slot == 0)

        @pl.when(from_here)
        def _():
            own.wait()

        @pl.when(jnp.logical_not(from_here))
        def _():
            onward(slot).wait_recv()

        stream = inbox[slot]
        projected = jnp.dot(stream, w_in[...], preferred_element_type=jnp.float32)
        projected = projected.astype(jnp.bfloat16).astype(jnp.float32)
        tap_count = taps.shape[0]
        convolved = cbias[...]
        for tap in range(tap_count):
            by = tap_count - 1 - tap
            shifted = delayed(projected, by, 0.0) if by else projected
            convolved = convolved + shifted * taps[tap : tap + 1]
        convolved = convolved.astype(jnp.bfloat16)

        def mapped(maps):
            return jnp.concatenate(
                [
                    jnp.dot(
                        convolved[:, i * wide : (i + 1) * wide],
                        maps[i],
                        preferred_element_type=jnp.float32,
                    )
                    for i in range(blocks // group)
                ],
                axis=1,
            )

        rate_gate = jax.nn.sigmoid(mapped(rate_map) + brate[...])
        input_gate = jax.nn.sigmoid(mapped(input_map) + binput[...])
        log_decay = rate_gate * dparam[...]
        decay = jnp.exp(log_decay)
        scale_in = jnp.sqrt(-jnp.tanh(log_decay) * (decay * decay + 1.0))
        hidden = scale_in * input_gate * convolved.astype(jnp.float32)
        by = 1
        while by < length:
            hidden = decay * delayed(hidden, by, 0.0) + hidden
            if 2 * by < length:
                decay = decay * delayed(decay, by, 1.0)
            by *= 2
        mixed = hidden.astype(jnp.bfloat16)
        summed = stream.astype(jnp.float32) + jnp.dot(
            mixed, w_out[...], preferred_element_type=jnp.float32
        )
        mean = jnp.mean(summed, axis=-1, keepdims=True)
        centered = summed - mean
        variance = jnp.mean(centered * centered, axis=-1, keepdims=True)
        normed = centered * lax.rsqrt(variance + norm_eps) * gain[...] + shift[...]
        result = normed.astype(jnp.bfloat16)
        outbox[slot] = result

        @pl.when(from_here)
        def _():
            pl.semaphore_wait(barrier, sections - 1)

        @pl.when(section < last)
        def _():
            onward(slot).start()

        @pl.when((section == last) & (slot < last))
        def _():
            home(slot).start()

        @pl.when((section == last) & (slot == last))
        def _():
            out_ref[0, 0] = outbox[slot]

        return carry

    lax.fori_loop(0, sections, one_slot, 0)

    @pl.when(section > 0)
    def _():
        entry.wait_send()

    @pl.when(section < last)
    def _():
        def sent(slot, carry):
            onward(slot).wait_send()
            return carry

        lax.fori_loop(0, sections, sent, 0)
        home(0).wait_recv()

    @pl.when(section == last)
    def _():
        def sent(slot, carry):
            home(slot).wait_send()
            return carry

        lax.fori_loop(0, last, sent, 0)


def shards(sections, tokens_in, *weights):
    _, _, length, width = tokens_in.shape
    lru_width = weights[0].shape[2]
    tap_count = weights[1].shape[1]
    _, blocks, block_width, _ = weights[3].shape
    group = max(1, min(blocks, mxu_width // block_width))
    wide = group * block_width
    vmem = pltpu.VMEM
    f32, bf16 = jnp.float32, jnp.bfloat16
    return pl.pallas_call(
        functools.partial(stack_kernel, sections),
        out_shape=jax.ShapeDtypeStruct(tokens_in.shape, tokens_in.dtype),
        in_specs=[pl.BlockSpec(memory_space=pl.ANY)] * (1 + len(weights)),
        out_specs=pl.BlockSpec(memory_space=pltpu.VMEM),
        scratch_shapes=[
            vmem((width, lru_width), bf16),
            vmem((lru_width, width), bf16),
            vmem((tap_count, lru_width), f32),
            vmem((1, lru_width), f32),
            vmem((blocks, block_width, block_width), bf16),
            vmem((1, lru_width), f32),
            vmem((blocks, block_width, block_width), bf16),
            vmem((1, lru_width), f32),
            vmem((1, lru_width), f32),
            vmem((1, width), f32),
            vmem((1, width), f32),
            vmem((blocks // group, wide, wide), bf16),
            vmem((blocks // group, wide, wide), bf16),
            vmem((sections, length, width), bf16),
            vmem((sections, length, width), bf16),
            pltpu.SemaphoreType.DMA((12,)),
            pltpu.SemaphoreType.DMA,
            pltpu.SemaphoreType.DMA((sections,)),
            pltpu.SemaphoreType.DMA((sections,)),
            pltpu.SemaphoreType.DMA,
        ],
        compiler_params=pltpu.CompilerParams(collective_id=0, has_side_effects=True),
        name="section_stack",
    )(tokens_in, *weights)


def solution(mesh):
    placed = (
        P("pp", ("fs", "tp"), None, None),
        P("pp", None, None),
        P("pp", None, None),
        P("pp", None),
        P("pp", None, None, None),
        P("pp", None),
        P("pp", None, None, None),
        P("pp", None),
        P("pp", None),
        P("pp", None, None),
        P("pp", None),
        P("pp", None),
    )
    return jax.shard_map(
        functools.partial(shards, mesh.shape["pp"]),
        mesh=mesh,
        in_specs=placed,
        out_specs=P("pp", ("fs", "tp"), None, None),
        check_vma=False,
    )
```

```python
import functools

import jax
import jax.numpy as jnp
from jax import lax
from jax.experimental import pallas as pl
from jax.experimental.pallas import tpu as pltpu
from jax.sharding import PartitionSpec as P

decay_scale = 8.0
norm_eps = 1e-05
mxu_width = 256
MESH = pl.DeviceIdType.MESH


def stack_kernel(
    sections,
    tokens_hbm,
    w_in_hbm,
    taps_hbm,
    cbias_hbm,
    grate_hbm,
    brate_hbm,
    ginput_hbm,
    binput_hbm,
    dparam_hbm,
    w_out_hbm,
    gain_hbm,
    shift_hbm,
    out_ref,
    w_in,
    w_out,
    taps,
    cbias,
    grate,
    brate,
    ginput,
    binput,
    dparam,
    gain,
    shift,
    rate_map,
    input_map,
    mine,
    inbox,
    outbox,
    load_sem,
    entry_sem,
    send_sem,
    recv_sem,
    final_sem,
):
    section = lax.axis_index("pp")
    column = lax.axis_index("tp")
    last = sections - 1
    pair, length = inbox.shape[1:3]
    lru_width = w_in.shape[1]
    core = lax.rem(column, pair)
    lead = pair - 1
    leads = core == lead
    first_stop = leads & (section == 0)
    last_stop = leads & (section == last)

    def at(stop, core_index):
        return {"pp": stop, "tp": column - core + core_index}

    barrier = pltpu.get_barrier_semaphore()

    def tell(stop, core_index):
        pl.semaphore_signal(
            barrier, inc=1, device_id=at(stop, core_index), device_id_type=MESH
        )

    @pl.when(first_stop)
    def _():
        for core_index in range(pair):
            for stop in range(sections):
                if (stop, core_index) != (0, lead):
                    tell(stop, core_index)

    @pl.when(jnp.logical_not(first_stop | last_stop))
    def _():
        tell(last, lead)

    @pl.when(leads & (section > 0))
    def _():
        @pl.when(section - 1 < last)
        def _():
            tell(section - 1, lead)

    heard = jnp.where(
        last_stop, sections * pair - 1, jnp.where(leads & (section > 0), 2, 1)
    ).astype(jnp.int32)

    def load(src, dst, index):
        return pltpu.make_async_copy(src, dst, load_sem.at[index])

    own = load(tokens_hbm.at[0, 0], mine, 0)
    load_in = load(w_in_hbm.at[0], w_in, 1)
    load_out = load(w_out_hbm.at[0], w_out, 2)
    small = [
        load(grate_hbm.at[0], grate, 3),
        load(ginput_hbm.at[0], ginput, 4),
        load(taps_hbm.at[0], taps, 5),
        load(cbias_hbm, cbias, 6),
        load(brate_hbm, brate, 7),
        load(binput_hbm, binput, 8),
        load(dparam_hbm, dparam, 9),
        load(gain_hbm, gain, 10),
        load(shift_hbm, shift, 11),
    ]
    own.start()

    @pl.when(leads)
    def _():
        for copy in small:
            copy.start()
        load_in.start()
        load_out.start()

    own.wait()
    entry = pltpu.make_async_remote_copy(
        src_ref=mine,
        dst_ref=inbox.at[section, core],
        send_sem=entry_sem,
        recv_sem=recv_sem.at[section, core],
        device_id=at(0, lead),
        device_id_type=MESH,
    )

    @pl.when(jnp.logical_not(first_stop))
    def _():
        pl.semaphore_wait(barrier, heard)
        entry.start()

    def entered(slot, core_index):
        return pltpu.make_async_remote_copy(
            src_ref=mine,
            dst_ref=inbox.at[slot, core_index],
            send_sem=entry_sem,
            recv_sem=recv_sem.at[slot, core_index],
            device_id=at(0, lead),
            device_id_type=MESH,
        )

    def onward(slot):
        return pltpu.make_async_remote_copy(
            src_ref=outbox.at[slot],
            dst_ref=inbox.at[slot],
            send_sem=send_sem.at[slot, 0],
            recv_sem=recv_sem.at[slot, 0],
            device_id=at(jnp.minimum(section + 1, last), lead),
            device_id_type=MESH,
        )

    def home(slot, core_index):
        return pltpu.make_async_remote_copy(
            src_ref=outbox.at[slot, core_index],
            dst_ref=out_ref.at[0, 0],
            send_sem=send_sem.at[slot, core_index],
            recv_sem=final_sem,
            device_id=at(slot, core_index),
            device_id_type=MESH,
        )

    def run_section():
        blocks, block_width, _ = grate.shape
        group = max(1, min(blocks, mxu_width // block_width))
        wide = group * block_width
        rate_map[...] = jnp.zeros_like(rate_map)
        input_map[...] = jnp.zeros_like(input_map)
        for copy in small:
            copy.wait()
        for block in range(blocks):
            to = (block % group) * block_width
            rate_map[block // group, to : to + block_width, to : to + block_width] = grate[block]
            input_map[block // group, to : to + block_width, to : to + block_width] = ginput[block]
        minus_decay = -dparam[...]
        softplus = jnp.maximum(minus_decay, 0.0) + jnp.log1p(jnp.exp(-jnp.abs(minus_decay)))
        dparam[...] = -decay_scale * softplus
        load_in.wait()
        load_out.wait()

        @pl.when(section == 0)
        def _():
            inbox[0, lead] = mine[...]

        position = lax.broadcasted_iota(jnp.int32, (pair, length, lru_width), 1)

        def delayed(x, by, fill):
            return jnp.where(position >= by, pltpu.roll(x, by, 1), fill)

        def one_slot(slot, carry):
            @pl.when(section == 0)
            def _():
                for core_index in range(pair):
                    if core_index == lead:
                        @pl.when(slot > 0)
                        def _():
                            entered(slot, core_index).wait_recv()
                    else:
                        entered(slot, core_index).wait_recv()

            @pl.when(section > 0)
            def _():
                onward(slot).wait_recv()

            rows = pair * length
            stream = inbox[slot].astype(jnp.float32).reshape(rows, -1)
            projected = jnp.dot(
                stream.astype(jnp.bfloat16), w_in[...], preferred_element_type=jnp.float32
            )
            projected = projected.astype(jnp.bfloat16).astype(jnp.float32)
            projected = projected.reshape(pair, length, lru_width)
            tap_count = taps.shape[0]
            convolved = cbias[...][None]
            for tap in range(tap_count):
                by = tap_count - 1 - tap
                shifted = delayed(projected, by, 0.0) if by else projected
                convolved = convolved + shifted * taps[tap : tap + 1][None]
            convolved = convolved.reshape(rows, lru_width).astype(jnp.bfloat16)

            def mapped(maps):
                return jnp.concatenate(
                    [
                        jnp.dot(
                            convolved[:, i * wide : (i + 1) * wide],
                            maps[i],
                            preferred_element_type=jnp.float32,
                        )
                        for i in range(blocks // group)
                    ],
                    axis=1,
                )

            rate_gate = jax.nn.sigmoid(mapped(rate_map) + brate[...])
            input_gate = jax.nn.sigmoid(mapped(input_map) + binput[...])
            log_decay = rate_gate * dparam[...]
            decay = jnp.exp(log_decay)
            scale_in = jnp.sqrt(-jnp.tanh(log_decay) * (decay * decay + 1.0))
            hidden = scale_in * input_gate * convolved.astype(jnp.float32)
            hidden = hidden.reshape(pair, length, lru_width)
            decay = decay.reshape(pair, length, lru_width)
            by = 1
            while by < length:
                hidden = decay * delayed(hidden, by, 0.0) + hidden
                if 2 * by < length:
                    decay = decay * delayed(decay, by, 1.0)
                by *= 2
            mixed = hidden.reshape(rows, lru_width).astype(jnp.bfloat16)
            summed = stream + jnp.dot(mixed, w_out[...], preferred_element_type=jnp.float32)
            mean = jnp.mean(summed, axis=-1, keepdims=True)
            centered = summed - mean
            variance = jnp.mean(centered * centered, axis=-1, keepdims=True)
            normed = centered * lax.rsqrt(variance + norm_eps) * gain[...] + shift[...]
            outbox[slot] = normed.reshape(pair, length, -1).astype(jnp.bfloat16)

            @pl.when((section == 0) & (slot == 0))
            def _():
                pl.semaphore_wait(barrier, heard)

            @pl.when(section < last)
            def _():
                onward(slot).start()

            @pl.when(section == last)
            def _():
                for core_index in range(pair):
                    if core_index == lead:
                        @pl.when(slot < last)
                        def _():
                            home(slot, core_index).start()

                        @pl.when(slot == last)
                        def _():
                            out_ref[0, 0] = outbox[slot, core_index]
                    else:
                        home(slot, core_index).start()

            return carry

        lax.fori_loop(0, sections, one_slot, 0)

        @pl.when(section < last)
        def _():
            def sent(slot, carry):
                onward(slot).wait_send()
                return carry

            lax.fori_loop(0, sections, sent, 0)

        @pl.when(section == last)
        def _():
            def sent(slot, carry):
                for core_index in range(pair):
                    if core_index == lead:
                        @pl.when(slot < last)
                        def _():
                            home(slot, core_index).wait_send()
                    else:
                        home(slot, core_index).wait_send()
                return carry

            lax.fori_loop(0, sections, sent, 0)

    pl.when(leads)(run_section)

    @pl.when(jnp.logical_not(first_stop))
    def _():
        entry.wait_send()

    @pl.when(jnp.logical_not(last_stop))
    def _():
        home(0, 0).wait_recv()


def shards(sections, pair, tokens_in, *weights):
    _, _, length, width = tokens_in.shape
    lru_width = weights[0].shape[2]
    tap_count = weights[1].shape[1]
    _, blocks, block_width, _ = weights[3].shape
    group = max(1, min(blocks, mxu_width // block_width))
    wide = group * block_width
    vmem = pltpu.VMEM
    f32, bf16 = jnp.float32, jnp.bfloat16
    return pl.pallas_call(
        functools.partial(stack_kernel, sections),
        out_shape=jax.ShapeDtypeStruct(tokens_in.shape, tokens_in.dtype),
        in_specs=[pl.BlockSpec(memory_space=pl.ANY)] * (1 + len(weights)),
        out_specs=pl.BlockSpec(memory_space=pltpu.VMEM),
        scratch_shapes=[
            vmem((width, lru_width), bf16),
            vmem((lru_width, width), bf16),
            vmem((tap_count, lru_width), f32),
            vmem((1, lru_width), f32),
            vmem((blocks, block_width, block_width), bf16),
            vmem((1, lru_width), f32),
            vmem((blocks, block_width, block_width), bf16),
            vmem((1, lru_width), f32),
            vmem((1, lru_width), f32),
            vmem((1, width), f32),
            vmem((1, width), f32),
            vmem((blocks // group, wide, wide), bf16),
            vmem((blocks // group, wide, wide), bf16),
            vmem((length, width), bf16),
            vmem((sections, pair, length, width), bf16),
            vmem((sections, pair, length, width), bf16),
            pltpu.SemaphoreType.DMA((12,)),
            pltpu.SemaphoreType.DMA,
            pltpu.SemaphoreType.DMA((sections, pair)),
            pltpu.SemaphoreType.DMA((sections, pair)),
            pltpu.SemaphoreType.DMA,
        ],
        compiler_params=pltpu.CompilerParams(collective_id=0, has_side_effects=True),
        name="section_stack",
    )(tokens_in, *weights)


def solution(mesh):
    placed = (
        P("pp", ("fs", "tp"), None, None),
        P("pp", None, None),
        P("pp", None, None),
        P("pp", None),
        P("pp", None, None, None),
        P("pp", None),
        P("pp", None, None, None),
        P("pp", None),
        P("pp", None),
        P("pp", None, None),
        P("pp", None),
        P("pp", None),
    )
    pair = 2 if mesh.shape["tp"] % 2 == 0 else 1
    return jax.shard_map(
        functools.partial(shards, mesh.shape["pp"], pair),
        mesh=mesh,
        in_specs=placed,
        out_specs=P("pp", ("fs", "tp"), None, None),
        check_vma=False,
    )
```

```python
import functools

import jax
import jax.numpy as jnp
from jax import lax
from jax.experimental import pallas as pl
from jax.experimental.pallas import tpu as pltpu
from jax.sharding import PartitionSpec as P

decay_scale = 8.0
norm_eps = 1e-05
mxu_width = 256
stream_parts = 4
MESH = pl.DeviceIdType.MESH


def stack_kernel(
    sections,
    tokens_hbm,
    w_in_hbm,
    taps_hbm,
    cbias_hbm,
    grate_hbm,
    brate_hbm,
    ginput_hbm,
    binput_hbm,
    dparam_hbm,
    w_out_hbm,
    gain_hbm,
    shift_hbm,
    out_ref,
    w_in,
    w_out,
    taps,
    cbias,
    grate,
    brate,
    ginput,
    binput,
    dparam,
    gain,
    shift,
    rate_map,
    input_map,
    mine,
    inbox,
    outbox,
    load_sem,
    entry_sem,
    send_sem,
    recv_sem,
    part_sem,
    final_sem,
):
    section = lax.axis_index("pp")
    column = lax.axis_index("tp")
    last = sections - 1
    pair, length = inbox.shape[1:3]
    width, lru_width = w_in.shape
    parts = part_sem.shape[1]
    core = lax.rem(column, pair)
    lead = pair - 1
    leads = core == lead
    first_stop = leads & (section == 0)
    last_stop = leads & (section == last)

    def at(stop, core_index):
        return {"pp": stop, "tp": column - core + core_index}

    barrier = pltpu.get_barrier_semaphore()

    def tell(stop, core_index):
        pl.semaphore_signal(
            barrier, inc=1, device_id=at(stop, core_index), device_id_type=MESH
        )

    @pl.when(first_stop)
    def _():
        for core_index in range(pair):
            for stop in range(sections):
                if (stop, core_index) != (0, lead):
                    tell(stop, core_index)

    @pl.when(jnp.logical_not(first_stop | last_stop))
    def _():
        tell(last, lead)

    @pl.when(leads & (section > 0))
    def _():
        @pl.when(section - 1 < last)
        def _():
            tell(section - 1, lead)

    heard = jnp.where(
        last_stop, sections * pair - 1, jnp.where(leads & (section > 0), 2, 1)
    ).astype(jnp.int32)

    def load(src, dst, index):
        return pltpu.make_async_copy(src, dst, load_sem.at[index])

    own = load(tokens_hbm.at[0, 0], mine, 0)
    load_in = load(w_in_hbm.at[0], w_in, 1)
    load_out = load(w_out_hbm.at[0], w_out, 2)
    small = [
        load(grate_hbm.at[0], grate, 3),
        load(ginput_hbm.at[0], ginput, 4),
        load(taps_hbm.at[0], taps, 5),
        load(cbias_hbm, cbias, 6),
        load(brate_hbm, brate, 7),
        load(binput_hbm, binput, 8),
        load(dparam_hbm, dparam, 9),
        load(gain_hbm, gain, 10),
        load(shift_hbm, shift, 11),
    ]
    own.start()

    @pl.when(leads)
    def _():
        for copy in small:
            copy.start()
        load_in.start()
        load_out.start()

    own.wait()
    entry = pltpu.make_async_remote_copy(
        src_ref=mine,
        dst_ref=inbox.at[section, core],
        send_sem=entry_sem,
        recv_sem=recv_sem.at[section, core],
        device_id=at(0, lead),
        device_id_type=MESH,
    )

    @pl.when(jnp.logical_not(first_stop))
    def _():
        pl.semaphore_wait(barrier, heard)
        entry.start()

    def entered(slot, core_index):
        return pltpu.make_async_remote_copy(
            src_ref=mine,
            dst_ref=inbox.at[slot, core_index],
            send_sem=entry_sem,
            recv_sem=recv_sem.at[slot, core_index],
            device_id=at(0, lead),
            device_id_type=MESH,
        )

    def onward(slot, part):
        across = slice(part * width // parts, (part + 1) * width // parts)
        return pltpu.make_async_remote_copy(
            src_ref=outbox.at[slot, :, :, across],
            dst_ref=inbox.at[slot, :, :, across],
            send_sem=send_sem.at[slot, part],
            recv_sem=part_sem.at[slot, part],
            device_id=at(jnp.minimum(section + 1, last), lead),
            device_id_type=MESH,
        )

    def home(slot, core_index):
        return pltpu.make_async_remote_copy(
            src_ref=outbox.at[slot, core_index],
            dst_ref=out_ref.at[0, 0],
            send_sem=send_sem.at[slot, core_index],
            recv_sem=final_sem,
            device_id=at(slot, core_index),
            device_id_type=MESH,
        )

    def run_section():
        blocks, block_width, _ = grate.shape
        group = max(1, min(blocks, mxu_width // block_width))
        wide = group * block_width
        rate_map[...] = jnp.zeros_like(rate_map)
        input_map[...] = jnp.zeros_like(input_map)
        for copy in small:
            copy.wait()
        for block in range(blocks):
            to = (block % group) * block_width
            rate_map[block // group, to : to + block_width, to : to + block_width] = grate[block]
            input_map[block // group, to : to + block_width, to : to + block_width] = ginput[block]
        minus_decay = -dparam[...]
        softplus = jnp.maximum(minus_decay, 0.0) + jnp.log1p(jnp.exp(-jnp.abs(minus_decay)))
        dparam[...] = -decay_scale * softplus
        load_in.wait()
        load_out.wait()

        @pl.when(section == 0)
        def _():
            inbox[0, lead] = mine[...]

        position = lax.broadcasted_iota(jnp.int32, (pair, length, lru_width), 1)

        def delayed(x, by, fill):
            return jnp.where(position >= by, pltpu.roll(x, by, 1), fill)

        def one_slot(slot, carry):
            @pl.when(section == 0)
            def _():
                for core_index in range(pair):
                    if core_index == lead:
                        @pl.when(slot > 0)
                        def _():
                            entered(slot, core_index).wait_recv()
                    else:
                        entered(slot, core_index).wait_recv()

            rows = pair * length
            projected = jnp.zeros((rows, lru_width), jnp.float32)
            streams = []
            for part in range(parts):
                @pl.when(section > 0)
                def _():
                    onward(slot, part).wait_recv()

                across = slice(part * width // parts, (part + 1) * width // parts)
                piece = inbox[slot, :, :, across].astype(jnp.float32).reshape(rows, -1)
                streams.append(piece)
                projected = projected + jnp.dot(
                    piece.astype(jnp.bfloat16),
                    w_in[across, :],
                    preferred_element_type=jnp.float32,
                )
            stream = jnp.concatenate(streams, axis=1)
            projected = projected.astype(jnp.bfloat16).astype(jnp.float32)
            projected = projected.reshape(pair, length, lru_width)
            tap_count = taps.shape[0]
            convolved = cbias[...][None]
            for tap in range(tap_count):
                by = tap_count - 1 - tap
                shifted = delayed(projected, by, 0.0) if by else projected
                convolved = convolved + shifted * taps[tap : tap + 1][None]
            convolved = convolved.reshape(rows, lru_width).astype(jnp.bfloat16)

            def mapped(maps):
                return jnp.concatenate(
                    [
                        jnp.dot(
                            convolved[:, i * wide : (i + 1) * wide],
                            maps[i],
                            preferred_element_type=jnp.float32,
                        )
                        for i in range(blocks // group)
                    ],
                    axis=1,
                )

            rate_gate = jax.nn.sigmoid(mapped(rate_map) + brate[...])
            input_gate = jax.nn.sigmoid(mapped(input_map) + binput[...])
            log_decay = rate_gate * dparam[...]
            decay = jnp.exp(log_decay)
            scale_in = jnp.sqrt(-jnp.tanh(log_decay) * (decay * decay + 1.0))
            hidden = scale_in * input_gate * convolved.astype(jnp.float32)
            hidden = hidden.reshape(pair, length, lru_width)
            decay = decay.reshape(pair, length, lru_width)
            by = 1
            while by < length:
                hidden = decay * delayed(hidden, by, 0.0) + hidden
                if 2 * by < length:
                    decay = decay * delayed(decay, by, 1.0)
                by *= 2
            mixed = hidden.reshape(rows, lru_width).astype(jnp.bfloat16)
            summed = stream + jnp.dot(mixed, w_out[...], preferred_element_type=jnp.float32)
            away = summed - jnp.mean(stream, axis=-1, keepdims=True)
            offset = jnp.mean(away, axis=-1, keepdims=True)
            square = jnp.mean(away * away, axis=-1, keepdims=True)
            variance = jnp.maximum(square - offset * offset, 0.0)
            normed = (away - offset) * lax.rsqrt(variance + norm_eps) * gain[...] + shift[...]
            outbox[slot] = normed.reshape(pair, length, -1).astype(jnp.bfloat16)

            @pl.when((section == 0) & (slot == 0))
            def _():
                pl.semaphore_wait(barrier, heard)

            @pl.when(section < last)
            def _():
                for part in range(parts):
                    onward(slot, part).start()

            @pl.when(section == last)
            def _():
                for core_index in range(pair):
                    if core_index == lead:
                        @pl.when(slot < last)
                        def _():
                            home(slot, core_index).start()

                        @pl.when(slot == last)
                        def _():
                            out_ref[0, 0] = outbox[slot, core_index]
                    else:
                        home(slot, core_index).start()

            return carry

        lax.fori_loop(0, sections, one_slot, 0)

        @pl.when(section < last)
        def _():
            def sent(slot, carry):
                for part in range(parts):
                    onward(slot, part).wait_send()
                return carry

            lax.fori_loop(0, sections, sent, 0)

        @pl.when(section == last)
        def _():
            def sent(slot, carry):
                for core_index in range(pair):
                    if core_index == lead:
                        @pl.when(slot < last)
                        def _():
                            home(slot, core_index).wait_send()
                    else:
                        home(slot, core_index).wait_send()
                return carry

            lax.fori_loop(0, sections, sent, 0)

    pl.when(leads)(run_section)

    @pl.when(jnp.logical_not(first_stop))
    def _():
        entry.wait_send()

    @pl.when(jnp.logical_not(last_stop))
    def _():
        home(0, 0).wait_recv()


def shards(sections, pair, tokens_in, *weights):
    _, _, length, width = tokens_in.shape
    lru_width = weights[0].shape[2]
    tap_count = weights[1].shape[1]
    _, blocks, block_width, _ = weights[3].shape
    group = max(1, min(blocks, mxu_width // block_width))
    wide = group * block_width
    vmem = pltpu.VMEM
    f32, bf16 = jnp.float32, jnp.bfloat16
    return pl.pallas_call(
        functools.partial(stack_kernel, sections),
        out_shape=pltpu.VMEM(tokens_in.shape, tokens_in.dtype),
        in_specs=[pl.BlockSpec(memory_space=pl.ANY)] * (1 + len(weights)),
        out_specs=pl.BlockSpec(memory_space=pltpu.VMEM),
        scratch_shapes=[
            vmem((width, lru_width), bf16),
            vmem((lru_width, width), bf16),
            vmem((tap_count, lru_width), f32),
            vmem((1, lru_width), f32),
            vmem((blocks, block_width, block_width), bf16),
            vmem((1, lru_width), f32),
            vmem((blocks, block_width, block_width), bf16),
            vmem((1, lru_width), f32),
            vmem((1, lru_width), f32),
            vmem((1, width), f32),
            vmem((1, width), f32),
            vmem((blocks // group, wide, wide), bf16),
            vmem((blocks // group, wide, wide), bf16),
            vmem((length, width), bf16),
            vmem((sections, pair, length, width), bf16),
            vmem((sections, pair, length, width), bf16),
            pltpu.SemaphoreType.DMA((12,)),
            pltpu.SemaphoreType.DMA,
            pltpu.SemaphoreType.DMA((sections, max(pair, stream_parts))),
            pltpu.SemaphoreType.DMA((sections, pair)),
            pltpu.SemaphoreType.DMA((sections, stream_parts)),
            pltpu.SemaphoreType.DMA,
        ],
        compiler_params=pltpu.CompilerParams(collective_id=0, has_side_effects=True),
        name="section_stack",
    )(tokens_in, *weights)


def solution(mesh):
    placed = (
        P("pp", ("fs", "tp"), None, None),
        P("pp", None, None),
        P("pp", None, None),
        P("pp", None),
        P("pp", None, None, None),
        P("pp", None),
        P("pp", None, None, None),
        P("pp", None),
        P("pp", None),
        P("pp", None, None),
        P("pp", None),
        P("pp", None),
    )
    pair = 2 if mesh.shape["tp"] % 2 == 0 else 1
    return jax.shard_map(
        functools.partial(shards, mesh.shape["pp"], pair),
        mesh=mesh,
        in_specs=placed,
        out_specs=P("pp", ("fs", "tp"), None, None),
        check_vma=False,
    )
```
